32 devices in a mesh: fs: 8 (over z, x), tp: 4 (over y, core).
Axes of the slice: x: 2, y: 2, z: 4, core: 2. Of those that a mesh axis runs over, the one named last changes fastest.
Arguments:
- tokens: bfloat16 [768, 4, 2048], P(None, 'tp'), may hold values from -6 to 6
- norm_gain: float32 [2048], P('fs'), may hold values from 0.1 to 1.9
- gate_weight: float32 [8, 2048, 4096], P(None, 'fs', 'tp'), may hold values from -0.125 to 0.125
- up_weight: float32 [8, 2048, 4096], P(None, 'fs', 'tp'), may hold values from -0.125 to 0.125
- down_weight: float32 [8, 2048, 4096], P(None, 'fs', 'tp'), may hold values from -0.09375 to 0.09375
- expert_ids: int32 [768, 4, 2], P(None, 'tp'), may hold values from 0 to 7, all different within a row
- expert_mix: float32 [768, 4, 2], P(None, 'tp'), may hold values from 0.2 to 1
Outputs:
- gate_serve: bfloat16 [8, 2048, 4096], P(None, None, 'fs')
- up_serve: bfloat16 [8, 2048, 4096], P(None, None, 'fs')
- down_serve: bfloat16 [8, 2048, 4096], P(None, None, 'fs')
- mixed: bfloat16 [768, 4, 2048], P('fs', 'tp')
The draws below stay inside these ranges and needn't reach their ends.
Inputs may be any that keep to these rules, and one draw needn't show every extreme that they name: `expert_ids`: each token names two different experts.
All inputs are finite; a program needn't handle non-finite values.
Results may differ from the reference program's by a relative error of at most 0.0082.
Values may be sent and summed in bfloat16 or wider, within the bound.
A program may use at most 192 MiB of HBM per device.

```python
import jax
import jax.numpy as jnp
from jax import lax

D = 2048
FF = 4096
EXPERTS = 8
ROWS = 768
N_TP = 4


def shard_levels(rng, shape, pieces, smallest, top_value):
    gain, own = 1.0, jax.random.fold_in(rng, 6)
    for axis_at, parts in pieces:
        heights = jnp.exp(jax.random.uniform(jax.random.fold_in(own, axis_at), (parts,), jnp.float32, smallest / len(pieces), top_value / len(pieces)))
        gain = gain * jnp.repeat(heights, shape[axis_at] // parts).reshape([-1 if axis == axis_at else 1 for axis in range(len(shape))])
    return gain


def picks_of(key, rows, count, top, lift):
    order = jax.random.permutation(jax.random.fold_in(key, 1), count)
    pull = order
    for power in range(3):
        pull = pull * pull // count
    pull = pull * lift // count
    tickets = jax.random.randint(jax.random.fold_in(key, 2), (rows, count), 0, 4096) + pull
    fixed_rows = jax.random.permutation(jax.random.fold_in(key, 3), rows)[jnp.arange(count) % rows]
    tickets = jnp.where(jnp.arange(rows)[:, None] == fixed_rows[None, :], 1 << 14, tickets)
    priority = tickets * count + jnp.arange(count)
    return lax.top_k(priority.astype(jnp.int32), top)[1].astype(jnp.int32)


def normal_values(rng, dims, deviation, reach, pieces=(), held_as=jnp.bfloat16):
    entries = jax.random.normal(rng, dims, jnp.float32) * deviation
    if len(pieces) > 0:
        entries = shard_levels(rng, dims, pieces, -0.22, 0.18) * entries
    return jnp.clip(entries, min=-reach, max=reach).astype(held_as)


def setup_inputs(seed: int = 0) -> dict:
    key_of = jax.random.split(jax.random.key(seed), 8)
    tokens = normal_values(key_of[0], (ROWS, N_TP, D), 1.0, 6.0, ((1, 4),))
    norm_gain = jnp.clip(1.0 + 0.18 * jax.random.normal(key_of[1], (D,), jnp.float32), 0.1, 1.9)
    gate_weight = normal_values(key_of[2], (EXPERTS, D, FF), D ** -0.5, 0.125, ((1, 8), (2, 4)), jnp.float32)
    up_weight = normal_values(key_of[3], (EXPERTS, D, FF), D ** -0.5, 0.125, ((1, 8), (2, 4)), jnp.float32)
    down_weight = normal_values(key_of[4], (EXPERTS, D, FF), FF ** -0.5, 0.09375, ((1, 8), (2, 4)), jnp.float32)
    expert_ids = picks_of(key_of[5], ROWS * N_TP, EXPERTS, 2, 0).reshape((ROWS, N_TP, 2))
    expert_mix = jnp.clip(0.2 + 0.8 * jax.random.uniform(key_of[6], (ROWS, N_TP, 2), jnp.float32) ** shard_levels(key_of[6], (ROWS, N_TP, 2), ((1, 4),), -0.2, 0.2), 0.2, 1.0)
    return dict(tokens=tokens, norm_gain=norm_gain, gate_weight=gate_weight, up_weight=up_weight, down_weight=down_weight, expert_ids=expert_ids, expert_mix=expert_mix)


norm_eps = 1e-05

def reference(tokens, norm_gain, gate_weight, up_weight, down_weight, expert_ids, expert_mix):
    gate_serve = (gate_weight * norm_gain[None, :, None]).astype(jnp.bfloat16)
    up_serve = (up_weight * norm_gain[None, :, None]).astype(jnp.bfloat16)
    down_serve = down_weight.astype(jnp.bfloat16)
    token_rows = tokens.reshape(-1, D).astype(jnp.float32)
    row_mean = lax.optimization_barrier(jnp.mean(token_rows, axis=1, keepdims=True))
    centered = token_rows - row_mean
    variance = lax.optimization_barrier(jnp.mean(centered * centered, axis=1, keepdims=True))
    normed = (centered * lax.rsqrt(variance + norm_eps)).astype(jnp.bfloat16)
    route_ids = expert_ids.reshape(-1, 2)
    route_mix = expert_mix.reshape(-1, 2)
    expert_iota = jnp.arange(EXPERTS, dtype=jnp.int32)
    expert_gates = lax.optimization_barrier(jnp.sum((route_ids[:, :, None] == expert_iota[None, None, :]).astype(jnp.float32) * route_mix[:, :, None], axis=1))

    def add_expert(running, weights_now):
        gate_mat, up_mat, down_mat, gate_col = weights_now
        gate_act = jnp.dot(normed, gate_mat, preferred_element_type=jnp.float32)
        up_act = jnp.dot(normed, up_mat, preferred_element_type=jnp.float32)
        hidden = (jax.nn.silu(gate_act) * up_act * gate_col[:, None]).astype(jnp.bfloat16)
        product = lax.dot_general(hidden, down_mat, (((1,), (1,)), ((), ())), preferred_element_type=jnp.float32)
        return (running + product, None)
    start_sum = jnp.zeros((token_rows.shape[0], D), jnp.float32)
    summed, _ = lax.scan(add_expert, start_sum, (gate_serve, up_serve, down_serve, expert_gates.T))
    mixed = summed.astype(jnp.bfloat16).reshape(ROWS, N_TP, D)
    return (gate_serve, up_serve, down_serve, mixed)
```

```python
import functools

import jax
import jax.numpy as jnp
from jax import lax
from jax.experimental import pallas as pl
from jax.experimental.pallas import tpu as pltpu
from jax.sharding import PartitionSpec as P

norm_eps = 1e-05
MESH = pl.DeviceIdType.MESH


def exchange_kernel(n_fs, n_tp, gate_in, up_in, down_in, gate_out, up_out, down_out, relay_buf,
                    hop_send, hop_recv, own_send, pass_send, core_send, side_send, land):
    ins, outs = (gate_in, up_in, down_in), (gate_out, up_out, down_out)
    experts, rows, columns = gate_in.shape
    per = n_fs // n_tp
    unit = columns // per
    f, t = lax.axis_index("fs"), lax.axis_index("tp")
    mate = t + 1 - 2 * lax.rem(t, 2)
    side = lax.rem(t + 2, n_tp)
    own = lax.div(f, per)
    own_mate = own + 1 - 2 * lax.rem(own, 2)
    near = t == own_mate
    far = t == lax.rem(own_mate + 2, n_tp)

    def hop(k, e):
        return pltpu.make_async_remote_copy(
            src_ref=ins[k].at[e], dst_ref=relay_buf.at[k - 1, e], send_sem=hop_send.at[k - 1, e],
            recv_sem=hop_recv.at[k - 1, e], device_id=(f, side), device_id_type=MESH)

    def straight(k, e, h):
        return pltpu.make_async_remote_copy(
            src_ref=ins[k].at[e, :, pl.ds(h * unit, unit)], dst_ref=outs[k].at[e, f], send_sem=own_send.at[k, e, h],
            recv_sem=land.at[k, e], device_id=(t * per + h, mate), device_id_type=MESH)

    def relayed(k, e, h):
        return pltpu.make_async_remote_copy(
            src_ref=relay_buf.at[k - 1, e, :, pl.ds(h * unit, unit)], dst_ref=outs[k].at[e, f],
            send_sem=pass_send.at[k - 1, e, h], recv_sem=land.at[k, e],
            device_id=(side * per + h, mate), device_id_type=MESH)

    def spread(k, e, to, sem):
        return pltpu.make_async_remote_copy(
            src_ref=outs[k].at[e], dst_ref=outs[k].at[e], send_sem=sem.at[k, e],
            recv_sem=land.at[k, e], device_id=(f, to), device_id_type=MESH)

    def to_mate(k, e):
        return spread(k, e, mate, core_send)

    def to_side(k, e):
        return spread(k, e, side, side_send)

    def landed(k, e):
        to_mate(k, e).wait_recv()

    def step(s, carry):
        @pl.when(s < experts)
        def _():
            hop(2, s).start()
            hop(1, s).start()
            for k in (0, 1):
                for h in range(per):
                    straight(k, s, h).start()

        @pl.when((s >= 1) & (s < experts + 1))
        def _():
            for k in (2, 1):
                hop(k, s - 1).wait_recv()
                for h in range(per):
                    relayed(k, s - 1, h).start()

        @pl.when((s >= 2) & (s < experts + 2))
        def _():
            e = s - 2

            @pl.when(near)
            def _():
                landed(0, e)
                to_side(0, e).start()
                to_mate(0, e).start()
                landed(1, e)
                to_mate(1, e).start()

            @pl.when(far)
            def _():
                landed(2, e)
                to_side(2, e).start()
                to_mate(2, e).start()
                landed(1, e)
                to_mate(1, e).start()

        @pl.when(s >= 3)
        def _():
            e = s - 3

            @pl.when(near)
            def _():
                landed(2, e)
                to_mate(2, e).start()

            @pl.when(far)
            def _():
                landed(0, e)
                to_mate(0, e).start()

        return carry

    lax.fori_loop(0, experts + 3, step, 0)

    def drain(e, carry):
        for k in (1, 2):
            hop(k, e).wait_send()
            for h in range(per):
                relayed(k, e, h).wait_send()
        for k in (0, 1):
            for h in range(per):
                straight(k, e, h).wait_send()

        @pl.when(near | far)
        def _():
            for k in range(3):
                to_mate(k, e).wait_send()

        @pl.when(near)
        def _():
            to_side(0, e).wait_send()

        @pl.when(far)
        def _():
            to_side(2, e).wait_send()

        @pl.when(jnp.logical_not(near | far))
        def _():
            for k in range(3):
                landed(k, e)

        return carry

    lax.fori_loop(0, experts, drain, 0)


def exchange(n_fs, n_tp, blocks):
    experts, rows, columns = blocks[0].shape
    per = n_fs // n_tp
    serve = jax.ShapeDtypeStruct((experts, n_fs, rows, columns // per), jnp.bfloat16)
    relay = jax.ShapeDtypeStruct((2, experts, rows, columns), jnp.bfloat16)
    dma = pltpu.SemaphoreType.DMA
    outs = pl.pallas_call(
        functools.partial(exchange_kernel, n_fs, n_tp),
        out_shape=(serve, serve, serve, relay),
        in_specs=[pl.BlockSpec(memory_space=pl.ANY)] * 3,
        out_specs=[pl.BlockSpec(memory_space=pl.ANY)] * 4,
        scratch_shapes=[
            dma((2, experts)),
            dma((2, experts)),
            dma((2, experts, per)),
            dma((2, experts, per)),
            dma((3, experts)),
            dma((3, experts)),
            dma((3, experts)),
        ],
        compiler_params=pltpu.CompilerParams(has_side_effects=True),
    )(*blocks)
    return tuple(out.reshape(experts, n_fs * rows, columns // per) for out in outs[:3])


def collective_exchange(blocks):
    regrouped = [lax.all_to_all(b, "tp", split_axis=0, concat_axis=2, tiled=True) for b in blocks]
    unit_split = [lax.all_to_all(b, "fs", split_axis=2, concat_axis=1, tiled=True) for b in regrouped]
    return tuple(lax.all_gather(b, "tp", axis=0, tiled=True) for b in unit_split)


def local(tokens, norm_gain, gate_weight, up_weight, down_weight, expert_ids, expert_mix):
    n_fs, n_tp = lax.axis_size("fs"), lax.axis_size("tp")
    blocks = (
        (gate_weight * norm_gain[None, :, None]).astype(jnp.bfloat16),
        (up_weight * norm_gain[None, :, None]).astype(jnp.bfloat16),
        down_weight.astype(jnp.bfloat16),
    )
    rows, columns = blocks[0].shape[1:]
    unit = columns * n_tp // n_fs
    if n_tp == 4 and n_fs % n_tp == 0 and unit % 128 == 0 and rows % 16 == 0:
        gate_serve, up_serve, down_serve = exchange(n_fs, n_tp, blocks)
    else:
        gate_serve, up_serve, down_serve = collective_exchange(blocks)
    width = tokens.shape[2]
    token_rows = tokens.reshape(-1, width).astype(jnp.float32)
    row_mean = jnp.mean(token_rows, axis=1, keepdims=True)
    centered = token_rows - row_mean
    variance = jnp.mean(centered * centered, axis=1, keepdims=True)
    normed = (centered * lax.rsqrt(variance + norm_eps)).astype(jnp.bfloat16)
    route_ids = expert_ids.reshape(-1, 2)
    route_mix = expert_mix.reshape(-1, 2)
    expert_iota = jnp.arange(gate_serve.shape[0], dtype=jnp.int32)
    expert_gates = jnp.sum(
        (route_ids[:, :, None] == expert_iota[None, None, :]).astype(jnp.float32)
        * route_mix[:, :, None],
        axis=1,
    )
    gate_act = jnp.einsum("rd,edf->ref", normed, gate_serve, preferred_element_type=jnp.float32)
    up_act = jnp.einsum("rd,edf->ref", normed, up_serve, preferred_element_type=jnp.float32)
    hidden = (jax.nn.silu(gate_act) * up_act * expert_gates[:, :, None]).astype(jnp.bfloat16)
    own_rows = token_rows.shape[0] // n_fs
    partial = jnp.einsum("ref,edf->rd", hidden, down_serve, preferred_element_type=jnp.float32)
    parts = partial.astype(jnp.bfloat16).reshape(n_fs, own_rows, width)
    parts = lax.all_to_all(parts, "fs", split_axis=0, concat_axis=0, tiled=True)
    summed = jnp.sum(parts.astype(jnp.float32), axis=0)
    mixed = summed.astype(jnp.bfloat16).reshape(own_rows, 1, width)
    return (gate_serve, up_serve, down_serve, mixed)


def solution(mesh):
    return jax.shard_map(
        local,
        mesh=mesh,
        in_specs=(
            P(None, "tp", None),
            P("fs"),
            P(None, "fs", "tp"),
            P(None, "fs", "tp"),
            P(None, "fs", "tp"),
            P(None, "tp", None),
            P(None, "tp", None),
        ),
        out_specs=(
            P(None, None, "fs"),
            P(None, None, "fs"),
            P(None, None, "fs"),
            P("fs", "tp", None),
        ),
        check_vma=False,
    )
```

```python
import functools

import jax
import jax.numpy as jnp
from jax import lax
from jax.experimental import pallas as pl
from jax.experimental.pallas import tpu as pltpu
from jax.sharding import PartitionSpec as P

norm_eps = 1e-05
MESH = pl.DeviceIdType.MESH


def exchange_kernel(n_fs, n_tp, gate_in, up_in, down_in, normed, gates, gate_out, up_out, down_out, relay_buf,
                    partial, held, total, hop_send, hop_recv, own_send, pass_send, core_send, side_send, land, load):
    ins, outs = (gate_in, up_in, down_in), (gate_out, up_out, down_out)
    experts, rows, columns = gate_in.shape
    per = n_fs // n_tp
    unit = columns // per
    f, t = lax.axis_index("fs"), lax.axis_index("tp")
    mate = t + 1 - 2 * lax.rem(t, 2)
    side = lax.rem(t + 2, n_tp)
    own = lax.div(f, per)
    own_mate = own + 1 - 2 * lax.rem(own, 2)
    near = t == own_mate
    far = t == lax.rem(own_mate + 2, n_tp)

    def hop(k, e):
        return pltpu.make_async_remote_copy(
            src_ref=ins[k].at[e], dst_ref=relay_buf.at[k - 1, e], send_sem=hop_send.at[k - 1, e],
            recv_sem=hop_recv.at[k - 1, e], device_id=(f, side), device_id_type=MESH)

    def straight(k, e, h):
        return pltpu.make_async_remote_copy(
            src_ref=ins[k].at[e, :, pl.ds(h * unit, unit)], dst_ref=outs[k].at[e, f], send_sem=own_send.at[k, e, h],
            recv_sem=land.at[k, e], device_id=(t * per + h, mate), device_id_type=MESH)

    def relayed(k, e, h):
        return pltpu.make_async_remote_copy(
            src_ref=relay_buf.at[k - 1, e, :, pl.ds(h * unit, unit)], dst_ref=outs[k].at[e, f],
            send_sem=pass_send.at[k - 1, e, h], recv_sem=land.at[k, e],
            device_id=(side * per + h, mate), device_id_type=MESH)

    def spread(k, e, to, sem):
        return pltpu.make_async_remote_copy(
            src_ref=outs[k].at[e], dst_ref=outs[k].at[e], send_sem=sem.at[k, e],
            recv_sem=land.at[k, e], device_id=(f, to), device_id_type=MESH)

    def to_mate(k, e):
        return spread(k, e, mate, core_send)

    def to_side(k, e):
        return spread(k, e, side, side_send)

    def landed(k, e):
        to_mate(k, e).wait_recv()

    tall = normed.shape[0] // 2
    deep = n_fs * rows

    def compute(e):
        loads = [pltpu.make_async_copy(outs[k].at[e], held.at[k], load.at[k]) for k in range(3)]
        for copy in loads:
            copy.start()
        for copy in loads:
            copy.wait()

        def some_rows(i, carry):
            now = pl.ds(pl.multiple_of(i * tall, tall), tall)
            tokens = normed[now, :]
            gate_act = jnp.dot(tokens, held[0].reshape(deep, unit), preferred_element_type=jnp.float32)
            up_act = jnp.dot(tokens, held[1].reshape(deep, unit), preferred_element_type=jnp.float32)
            hidden = gate_act / (1.0 + jnp.exp(-gate_act)) * up_act * gates[e, now, :]
            total[now, :] += lax.dot_general(
                hidden.astype(jnp.bfloat16), held[2].reshape(deep, unit), (((1,), (1,)), ((), ())),
                preferred_element_type=jnp.float32)
            return carry

        lax.fori_loop(0, 2, some_rows, 0)

    total[...] = jnp.zeros_like(total)

    def step(s, carry):
        @pl.when(s < experts)
        def _():
            hop(2, s).start()
            hop(1, s).start()
            for k in (0, 1):
                for h in range(per):
                    straight(k, s, h).start()

        @pl.when((s >= 1) & (s < experts + 1))
        def _():
            for k in (2, 1):
                hop(k, s - 1).wait_recv()
                for h in range(per):
                    relayed(k, s - 1, h).start()

        @pl.when((s >= 2) & (s < experts + 2))
        def _():
            e = s - 2

            @pl.when(near)
            def _():
                landed(0, e)
                to_side(0, e).start()
                to_mate(0, e).start()
                landed(1, e)
                to_mate(1, e).start()

            @pl.when(far)
            def _():
                landed(2, e)
                to_side(2, e).start()
                to_mate(2, e).start()
                landed(1, e)
                to_mate(1, e).start()

        @pl.when(s >= 3)
        def _():
            e = s - 3

            @pl.when(near)
            def _():
                landed(2, e)
                to_mate(2, e).start()

            @pl.when(far)
            def _():
                landed(0, e)
                to_mate(0, e).start()

            @pl.when(jnp.logical_not(near | far))
            def _():
                for k in range(3):
                    landed(k, e)

            compute(e)

        return carry

    lax.fori_loop(0, experts + 3, step, 0)
    partial[...] = total[...].astype(jnp.bfloat16)

    def drain(e, carry):
        for k in (1, 2):
            hop(k, e).wait_send()
            for h in range(per):
                relayed(k, e, h).wait_send()
        for k in (0, 1):
            for h in range(per):
                straight(k, e, h).wait_send()

        @pl.when(near | far)
        def _():
            for k in range(3):
                to_mate(k, e).wait_send()

        @pl.when(near)
        def _():
            to_side(0, e).wait_send()

        @pl.when(far)
        def _():
            to_side(2, e).wait_send()

        return carry

    lax.fori_loop(0, experts, drain, 0)


def exchange(n_fs, n_tp, blocks, normed, gates):
    experts, rows, columns = blocks[0].shape
    per = n_fs // n_tp
    serve = jax.ShapeDtypeStruct((experts, n_fs, rows, columns // per), jnp.bfloat16)
    relay = jax.ShapeDtypeStruct((2, experts, rows, columns), jnp.bfloat16)
    dma = pltpu.SemaphoreType.DMA
    outs = pl.pallas_call(
        functools.partial(exchange_kernel, n_fs, n_tp),
        out_shape=(serve, serve, serve, relay, jax.ShapeDtypeStruct(normed.shape, jnp.bfloat16)),
        in_specs=[pl.BlockSpec(memory_space=pl.ANY)] * 3 + [pl.BlockSpec(memory_space=pltpu.VMEM)] * 2,
        out_specs=[pl.BlockSpec(memory_space=pl.ANY)] * 4 + [pl.BlockSpec(memory_space=pltpu.VMEM)],
        scratch_shapes=[
            pltpu.VMEM((3, n_fs, rows, columns // per), jnp.bfloat16),
            pltpu.VMEM(normed.shape, jnp.float32),
            dma((2, experts)),
            dma((2, experts)),
            dma((2, experts, per)),
            dma((2, experts, per)),
            dma((3, experts)),
            dma((3, experts)),
            dma((3, experts)),
            dma((3,)),
        ],
        compiler_params=pltpu.CompilerParams(has_side_effects=True, vmem_limit_bytes=60 * 1024 * 1024),
    )(*blocks, normed, gates.T[:, :, None])
    return tuple(out.reshape(experts, n_fs * rows, columns // per) for out in outs[:3]) + (outs[4],)


def copy_kernel(*refs):
    half = len(refs) // 2
    for source, target in zip(refs[:half], refs[half:]):
        target[...] = source[...]


def copied(arrays):
    experts, deep, unit = arrays[0].shape
    block = pl.BlockSpec((1, deep, unit), lambda e: (e, 0, 0))
    return pl.pallas_call(
        copy_kernel,
        grid=(experts,),
        out_shape=tuple(jax.ShapeDtypeStruct(a.shape, a.dtype) for a in arrays),
        in_specs=[block] * len(arrays),
        out_specs=[block] * len(arrays),
        cost_estimate=pl.CostEstimate(flops=0, bytes_accessed=4 * len(arrays) * arrays[0].size, transcendentals=0),
        compiler_params=pltpu.CompilerParams(vmem_limit_bytes=40 * 1024 * 1024),
    )(*arrays)


def collective_exchange(blocks):
    regrouped = [lax.all_to_all(b, "tp", split_axis=0, concat_axis=2, tiled=True) for b in blocks]
    unit_split = [lax.all_to_all(b, "fs", split_axis=2, concat_axis=1, tiled=True) for b in regrouped]
    return tuple(lax.all_gather(b, "tp", axis=0, tiled=True) for b in unit_split)


def expert_layer(normed, expert_gates, gate_serve, up_serve, down_serve):
    gate_act = jnp.einsum("rd,edf->ref", normed, gate_serve, preferred_element_type=jnp.float32)
    up_act = jnp.einsum("rd,edf->ref", normed, up_serve, preferred_element_type=jnp.float32)
    hidden = (jax.nn.silu(gate_act) * up_act * expert_gates[:, :, None]).astype(jnp.bfloat16)
    return jnp.einsum("ref,edf->rd", hidden, down_serve, preferred_element_type=jnp.float32).astype(jnp.bfloat16)


def sum_parts(parts, n_fs):
    if n_fs > 8:
        parts = lax.all_to_all(parts, "fs", split_axis=0, concat_axis=0, tiled=True)
        return jnp.sum(parts.astype(jnp.float32), axis=0)
    f = lax.axis_index("fs")
    got = [lax.dynamic_index_in_dim(parts, f, 0, keepdims=False)]
    for j in range(1, n_fs):
        mine = lax.dynamic_index_in_dim(parts, lax.rem(f + j, n_fs), 0, keepdims=False)
        got.append(lax.ppermute(mine, "fs", [(i, (i + j) % n_fs) for i in range(n_fs)]))
    return sum(g.astype(jnp.float32) for g in got)


def local(tokens, norm_gain, gate_weight, up_weight, down_weight, expert_ids, expert_mix):
    n_fs, n_tp = lax.axis_size("fs"), lax.axis_size("tp")
    blocks = (
        (gate_weight * norm_gain[None, :, None]).astype(jnp.bfloat16),
        (up_weight * norm_gain[None, :, None]).astype(jnp.bfloat16),
        down_weight.astype(jnp.bfloat16),
    )
    width = tokens.shape[2]
    token_rows = tokens.reshape(-1, width).astype(jnp.float32)
    row_mean = jnp.mean(token_rows, axis=1, keepdims=True)
    centered = token_rows - row_mean
    variance = jnp.mean(centered * centered, axis=1, keepdims=True)
    normed = (centered * lax.rsqrt(variance + norm_eps)).astype(jnp.bfloat16)
    route_ids = expert_ids.reshape(-1, 2)
    route_mix = expert_mix.reshape(-1, 2)
    expert_iota = jnp.arange(gate_weight.shape[0], dtype=jnp.int32)
    expert_gates = jnp.sum(
        (route_ids[:, :, None] == expert_iota[None, None, :]).astype(jnp.float32)
        * route_mix[:, :, None],
        axis=1,
    )
    rows, columns = blocks[0].shape[1:]
    unit = columns * n_tp // n_fs
    halves = token_rows.shape[0] % 32 == 0
    if n_tp == 4 and n_fs % n_tp == 0 and unit % 128 == 0 and rows % 16 == 0 and halves:
        gate_serve, up_serve, down_serve, partial = exchange(n_fs, n_tp, blocks, normed, expert_gates)
        gate_serve, up_serve, down_serve = copied((gate_serve, up_serve, down_serve))
    else:
        gate_serve, up_serve, down_serve = collective_exchange(blocks)
        partial = expert_layer(normed, expert_gates, gate_serve, up_serve, down_serve)
    own_rows = token_rows.shape[0] // n_fs
    summed = sum_parts(partial.reshape(n_fs, own_rows, width), n_fs)
    mixed = summed.astype(jnp.bfloat16).reshape(own_rows, 1, width)
    return (gate_serve, up_serve, down_serve, mixed)


def solution(mesh):
    return jax.shard_map(
        local,
        mesh=mesh,
        in_specs=(
            P(None, "tp", None),
            P("fs"),
            P(None, "fs", "tp"),
            P(None, "fs", "tp"),
            P(None, "fs", "tp"),
            P(None, "tp", None),
            P(None, "tp", None),
        ),
        out_specs=(
            P(None, None, "fs"),
            P(None, None, "fs"),
            P(None, None, "fs"),
            P("fs", "tp", None),
        ),
        check_vma=False,
    )
```

```python
import functools

import jax
import jax.numpy as jnp
from jax import lax
from jax.experimental import pallas as pl
from jax.experimental.pallas import tpu as pltpu
from jax.sharding import PartitionSpec as P

norm_eps = 1e-05
MESH = pl.DeviceIdType.MESH


def exchange_kernel(n_fs, n_tp, gate_in, up_in, down_in, normed, gates, gate_out, up_out, down_out, relay_buf,
                    partial, held, total, hop_send, hop_recv, own_send, pass_send, core_send, side_send, land, load):
    ins, outs = (gate_in, up_in, down_in), (gate_out, up_out, down_out)
    experts, rows, columns = gate_in.shape
    per = n_fs // n_tp
    unit = columns // per
    f, t = lax.axis_index("fs"), lax.axis_index("tp")
    mate = t + 1 - 2 * lax.rem(t, 2)
    side = lax.rem(t + 2, n_tp)
    own = lax.div(f, per)
    own_mate = own + 1 - 2 * lax.rem(own, 2)
    near = t == own_mate
    far = t == lax.rem(own_mate + 2, n_tp)

    def hop(k, e):
        return pltpu.make_async_remote_copy(
            src_ref=ins[k].at[e], dst_ref=relay_buf.at[k - 1, e], send_sem=hop_send.at[k - 1, e],
            recv_sem=hop_recv.at[k - 1, e], device_id=(f, side), device_id_type=MESH)

    def straight(k, e, h):
        return pltpu.make_async_remote_copy(
            src_ref=ins[k].at[e, :, pl.ds(h * unit, unit)], dst_ref=outs[k].at[e, f], send_sem=own_send.at[k, e, h],
            recv_sem=land.at[k, e], device_id=(t * per + h, mate), device_id_type=MESH)

    def relayed(k, e, h):
        return pltpu.make_async_remote_copy(
            src_ref=relay_buf.at[k - 1, e, :, pl.ds(h * unit, unit)], dst_ref=outs[k].at[e, f],
            send_sem=pass_send.at[k - 1, e, h], recv_sem=land.at[k, e],
            device_id=(side * per + h, mate), device_id_type=MESH)

    def spread(k, e, to, sem):
        return pltpu.make_async_remote_copy(
            src_ref=outs[k].at[e], dst_ref=outs[k].at[e], send_sem=sem.at[k, e],
            recv_sem=land.at[k, e], device_id=(f, to), device_id_type=MESH)

    def to_mate(k, e):
        return spread(k, e, mate, core_send)

    def to_side(k, e):
        return spread(k, e, side, side_send)

    def landed(k, e):
        to_mate(k, e).wait_recv()

    tall = normed.shape[0] // 2
    deep = n_fs * rows

    def compute(e):
        loads = [pltpu.make_async_copy(outs[k].at[e], held.at[k], load.at[k]) for k in range(3)]
        for copy in loads:
            copy.start()
        for copy in loads:
            copy.wait()

        def some_rows(i, carry):
            now = pl.ds(pl.multiple_of(i * tall, tall), tall)
            tokens = normed[now, :]
            gate_act = jnp.dot(tokens, held[0].reshape(deep, unit), preferred_element_type=jnp.float32)
            up_act = jnp.dot(tokens, held[1].reshape(deep, unit), preferred_element_type=jnp.float32)
            hidden = gate_act / (1.0 + jnp.exp(-gate_act)) * up_act * gates[e, now, :]
            total[now, :] += lax.dot_general(
                hidden.astype(jnp.bfloat16), held[2].reshape(deep, unit), (((1,), (1,)), ((), ())),
                preferred_element_type=jnp.float32)
            return carry

        lax.fori_loop(0, 2, some_rows, 0)

    total[...] = jnp.zeros_like(total)

    def step(s, carry):
        @pl.when(s < experts)
        def _():
            hop(2, s).start()
            hop(1, s).start()
            for k in (0, 1):
                for h in range(per):
                    straight(k, s, h).start()

        @pl.when((s >= 1) & (s < experts + 1))
        def _():
            for k in (2, 1):
                hop(k, s - 1).wait_recv()
                for h in range(per):
                    relayed(k, s - 1, h).start()

        @pl.when((s >= 3) & (s < experts + 3))
        def _():
            e = s - 3

            @pl.when(near)
            def _():
                landed(0, e)
                to_side(0, e).start()
                to_mate(0, e).start()
                landed(1, e)
                to_mate(1, e).start()

            @pl.when(far)
            def _():
                landed(2, e)
                to_side(2, e).start()
                to_mate(2, e).start()
                landed(1, e)
                to_mate(1, e).start()

        @pl.when(s >= 4)
        def _():
            e = s - 4

            @pl.when(near)
            def _():
                landed(2, e)
                to_mate(2, e).start()

            @pl.when(far)
            def _():
                landed(0, e)
                to_mate(0, e).start()

            @pl.when(jnp.logical_not(near | far))
            def _():
                for k in range(3):
                    landed(k, e)

            compute(e)

        return carry

    lax.fori_loop(0, experts + 4, step, 0)
    partial[...] = total[...].astype(jnp.bfloat16)

    def drain(e, carry):
        for k in (1, 2):
            hop(k, e).wait_send()
            for h in range(per):
                relayed(k, e, h).wait_send()
        for k in (0, 1):
            for h in range(per):
                straight(k, e, h).wait_send()

        @pl.when(near | far)
        def _():
            for k in range(3):
                to_mate(k, e).wait_send()

        @pl.when(near)
        def _():
            to_side(0, e).wait_send()

        @pl.when(far)
        def _():
            to_side(2, e).wait_send()

        return carry

    lax.fori_loop(0, experts, drain, 0)


def exchange(n_fs, n_tp, blocks, normed, gates):
    experts, rows, columns = blocks[0].shape
    per = n_fs // n_tp
    serve = jax.ShapeDtypeStruct((experts, n_fs, rows, columns // per), jnp.bfloat16)
    relay = jax.ShapeDtypeStruct((2, experts, rows, columns), jnp.bfloat16)
    dma = pltpu.SemaphoreType.DMA
    outs = pl.pallas_call(
        functools.partial(exchange_kernel, n_fs, n_tp),
        out_shape=(serve, serve, serve, relay, jax.ShapeDtypeStruct(normed.shape, jnp.bfloat16)),
        in_specs=[pl.BlockSpec(memory_space=pl.ANY)] * 3 + [pl.BlockSpec(memory_space=pltpu.VMEM)] * 2,
        out_specs=[pl.BlockSpec(memory_space=pl.ANY)] * 4 + [pl.BlockSpec(memory_space=pltpu.VMEM)],
        scratch_shapes=[
            pltpu.VMEM((3, n_fs, rows, columns // per), jnp.bfloat16),
            pltpu.VMEM(normed.shape, jnp.float32),
            dma((2, experts)),
            dma((2, experts)),
            dma((2, experts, per)),
            dma((2, experts, per)),
            dma((3, experts)),
            dma((3, experts)),
            dma((3, experts)),
            dma((3,)),
        ],
        compiler_params=pltpu.CompilerParams(has_side_effects=True, vmem_limit_bytes=60 * 1024 * 1024),
    )(*blocks, normed, gates.T[:, :, None])
    return tuple(out.reshape(experts, n_fs * rows, columns // per) for out in outs[:3]) + (outs[4],)


def copy_kernel(*refs):
    half = len(refs) // 2
    for source, target in zip(refs[:half], refs[half:]):
        target[...] = source[...]


def copied(arrays):
    experts, deep, unit = arrays[0].shape
    block = pl.BlockSpec((1, deep, unit), lambda e: (e, 0, 0))
    return pl.pallas_call(
        copy_kernel,
        grid=(experts,),
        out_shape=tuple(jax.ShapeDtypeStruct(a.shape, a.dtype) for a in arrays),
        in_specs=[block] * len(arrays),
        out_specs=[block] * len(arrays),
        cost_estimate=pl.CostEstimate(flops=0, bytes_accessed=4 * len(arrays) * arrays[0].size, transcendentals=0),
        compiler_params=pltpu.CompilerParams(vmem_limit_bytes=40 * 1024 * 1024),
    )(*arrays)


def collective_exchange(blocks):
    regrouped = [lax.all_to_all(b, "tp", split_axis=0, concat_axis=2, tiled=True) for b in blocks]
    unit_split = [lax.all_to_all(b, "fs", split_axis=2, concat_axis=1, tiled=True) for b in regrouped]
    return tuple(lax.all_gather(b, "tp", axis=0, tiled=True) for b in unit_split)


def expert_layer(normed, expert_gates, gate_serve, up_serve, down_serve):
    gate_act = jnp.einsum("rd,edf->ref", normed, gate_serve, preferred_element_type=jnp.float32)
    up_act = jnp.einsum("rd,edf->ref", normed, up_serve, preferred_element_type=jnp.float32)
    hidden = (jax.nn.silu(gate_act) * up_act * expert_gates[:, :, None]).astype(jnp.bfloat16)
    return jnp.einsum("ref,edf->rd", hidden, down_serve, preferred_element_type=jnp.float32).astype(jnp.bfloat16)


def sum_parts(parts, n_fs):
    if n_fs > 8:
        parts = lax.all_to_all(parts, "fs", split_axis=0, concat_axis=0, tiled=True)
        return jnp.sum(parts.astype(jnp.float32), axis=0)
    f = lax.axis_index("fs")
    got = [lax.dynamic_index_in_dim(parts, f, 0, keepdims=False)]
    for j in range(1, n_fs):
        mine = lax.dynamic_index_in_dim(parts, lax.rem(f + j, n_fs), 0, keepdims=False)
        got.append(lax.ppermute(mine, "fs", [(i, (i + j) % n_fs) for i in range(n_fs)]))
    return sum(g.astype(jnp.float32) for g in got)


def local(tokens, norm_gain, gate_weight, up_weight, down_weight, expert_ids, expert_mix):
    n_fs, n_tp = lax.axis_size("fs"), lax.axis_size("tp")
    blocks = (
        (gate_weight * norm_gain[None, :, None]).astype(jnp.bfloat16),
        (up_weight * norm_gain[None, :, None]).astype(jnp.bfloat16),
        down_weight.astype(jnp.bfloat16),
    )
    width = tokens.shape[2]
    token_rows = tokens.reshape(-1, width).astype(jnp.float32)
    row_mean = jnp.mean(token_rows, axis=1, keepdims=True)
    centered = token_rows - row_mean
    variance = jnp.mean(centered * centered, axis=1, keepdims=True)
    normed = (centered * lax.rsqrt(variance + norm_eps)).astype(jnp.bfloat16)
    route_ids = expert_ids.reshape(-1, 2)
    route_mix = expert_mix.reshape(-1, 2)
    expert_iota = jnp.arange(gate_weight.shape[0], dtype=jnp.int32)
    expert_gates = jnp.sum(
        (route_ids[:, :, None] == expert_iota[None, None, :]).astype(jnp.float32)
        * route_mix[:, :, None],
        axis=1,
    )
    rows, columns = blocks[0].shape[1:]
    unit = columns * n_tp // n_fs
    halves = token_rows.shape[0] % 32 == 0
    if n_tp == 4 and n_fs % n_tp == 0 and unit % 128 == 0 and rows % 16 == 0 and halves:
        gate_serve, up_serve, down_serve, partial = exchange(n_fs, n_tp, blocks, normed, expert_gates)
        gate_serve, up_serve, down_serve = copied((gate_serve, up_serve, down_serve))
    else:
        gate_serve, up_serve, down_serve = collective_exchange(blocks)
        partial = expert_layer(normed, expert_gates, gate_serve, up_serve, down_serve)
    own_rows = token_rows.shape[0] // n_fs
    summed = sum_parts(partial.reshape(n_fs, own_rows, width), n_fs)
    mixed = summed.astype(jnp.bfloat16).reshape(own_rows, 1, width)
    return (gate_serve, up_serve, down_serve, mixed)


def solution(mesh):
    return jax.shard_map(
        local,
        mesh=mesh,
        in_specs=(
            P(None, "tp", None),
            P("fs"),
            P(None, "fs", "tp"),
            P(None, "fs", "tp"),
            P(None, "fs", "tp"),
            P(None, "tp", None),
            P(None, "tp", None),
        ),
        out_specs=(
            P(None, None, "fs"),
            P(None, None, "fs"),
            P(None, None, "fs"),
            P("fs", "tp", None),
        ),
        check_vma=False,
    )
```
